32 devices in a mesh: grp: 2 (over x), ep: 16 (over z, y, core).
Axes of the slice: x: 2, y: 2, z: 4, core: 2. Of those that a mesh axis runs over, the one named last changes fastest.
Arguments:
- tokens: bfloat16 [4096, 2048], P(('grp', 'ep')), parts along dimension 0, may hold values from -6 to 6
- routing: int32 [4096, 2], P(('grp', 'ep')), parts along dimension 0, may hold values from 0 to 3, all different within a row; in each aligned block of 128 rows (0 to 127, 128 to 255, ...) at most 80 rows name the same one
- gates: float32 [4096, 2], P(('grp', 'ep')), parts along dimension 0, may hold values from 0.2 to 1
- norm_gain: bfloat16 [2048], replicated, may hold values from 0.099609375 to 1.8984375
- w_gate: bfloat16 [16, 2048, 896], P('ep'), may hold values from -0.125 to 0.125
- w_up: bfloat16 [16, 2048, 896], P('ep'), may hold values from -0.125 to 0.125
- w_down: bfloat16 [16, 896, 2048], P('ep'), may hold values from -0.09375 to 0.09375
Outputs:
- mixed: bfloat16 [4096, 2048], P(('grp', 'ep')), parts along dimension 0
The draws below stay inside these ranges and needn't reach their ends.
There are 2 independent parts, one for each index of `grp`. The reference program is written for one: setup_inputs(seed, part) draws one part's arguments, and reference() takes and returns one part's arrays. A program takes and returns all parts, laid end to end along the dimension named above; an argument that names none is the same for every part. Nothing has to cross between parts.
Inputs may be any that keep to these rules, and one draw needn't show every extreme that they name: `routing`: each row names 2 different experts. Among the rows of one device at most 80 name any one expert, and in every draw some expert is named by exactly 80 rows of some device.
All inputs are finite; a program needn't handle non-finite values.
Results may differ from the reference program's by a relative error of at most 0.0078.
Values may be sent and summed in bfloat16 or wider, within the bound.
A program may use at most 128 MiB of HBM per device.

```python
import math
import jax
import jax.numpy as jnp
import numpy as np
from jax import lax

D = 2048
FF = 3584
TOP = 2
GROUP = 4
TOK_DEV = 128
EXPERTS = 4
CAP = 80
TOKENS = 2048
N_EP = 16


def levels(key, dims, pieces, low, top_value):
    factor_of, own = 1.0, jax.random.fold_in(key, 6)
    for axis_at, blocks in pieces:
        steps = jnp.exp(jax.random.uniform(jax.random.fold_in(own, axis_at), (blocks,), jnp.float32, low / len(pieces), top_value / len(pieces)))
        factor_of = factor_of * jnp.repeat(steps, dims[axis_at] // blocks).reshape([-1 if axis == axis_at else 1 for axis in range(len(dims))])
    return factor_of


def assign_block(own_key, own, number, rows, number_of, top, bound, lean):
    order = jax.random.permutation(own_key, number_of)
    heavy_load, common = load_shares(number_of, rows * top, bound, lean, True), load_shares(number_of, rows * top, bound, lean, False)
    places = jnp.arange(number_of)

    def named(sizes, offset_by):
        used = int((sizes > 0).sum())
        fixed = max(1, used // 4)
        passed = fixed + (places - fixed + offset_by * (used - fixed)) % max(1, number_of - fixed)
        return jnp.zeros((number_of,), jnp.int32).at[order[jnp.where(places < fixed, places, passed)]].set(jnp.asarray(sizes, jnp.int32))

    sizes = jnp.where(number % 4 == 0, named(heavy_load, number // 4), named(common, number - number // 4 - 1))
    mixed = jax.random.permutation(jax.random.fold_in(own, 3), number_of)
    donor, taker = mixed[0:number_of // 2 * 2:2], mixed[1:number_of // 2 * 2:2]
    room = jnp.minimum(sizes[donor] - 1, bound - sizes[taker]) // 2
    room = jnp.where((donor == order[0]) | (taker == order[0]) | (sizes[taker] == 0), 0, jnp.maximum(room, 0))
    passed = jax.random.randint(jax.random.fold_in(own, 4), (number_of // 2,), 0, 1 << 20) % (room + 1)
    sizes = sizes.at[donor].add(-passed).at[taker].add(passed)
    labels = jnp.searchsorted(jnp.cumsum(sizes), jnp.arange(rows * top), side="right").astype(jnp.int32)
    table = labels.reshape(top, rows).T
    table = table[jax.random.permutation(jax.random.fold_in(own, 1), rows)]
    offset_by = jax.random.randint(jax.random.fold_in(own, 2), (rows, 1), 0, top)
    return jnp.take_along_axis(table, (jnp.arange(top)[None, :] + offset_by) % top, axis=1)


def load_shares(number_of, total, bound, skew, full):
    portions = [(1 << 20) // math.isqrt(grade ** skew) + 1 for grade in range(1, number_of + 1)]
    largest = bound if full else min(bound, max(-(-total // number_of), total * portions[0] // sum(portions)))
    least = 1 if total - largest >= number_of - 1 else 0
    given, spare = [largest] + [least] * (number_of - 1), total - largest - least * (number_of - 1)
    while spare > 0:
        free = [i for i in range(1, number_of) if given[i] < largest] or [i for i in range(1, number_of) if given[i] < bound]
        pool, left = sum([portions[i] for i in free]), spare
        for i in free:
            extra = min(bound - given[i], max(1, left * portions[i] // pool), spare)
            given[i] = given[i] + extra
            spare = spare - extra
    return np.array(given)


def normal_values(rng, shape, deviation, limit, pieces=(), kind=jnp.bfloat16):
    values = deviation * jax.random.normal(rng, shape, jnp.float32)
    if pieces:
        values = values * levels(rng, shape, pieces, -0.22, 0.18)
    return jnp.clip(values, -limit, limit).astype(kind)


def setup_inputs(seed: int = 0, part: int = 0) -> dict:
    key_of = jax.random.split(jax.random.key(seed), 8)
    own_keys = jax.random.split(jax.random.fold_in(key_of[7], part), 8)
    tokens = normal_values(own_keys[0], (TOKENS, D), 1.0, 6.0, ((0, 16),))
    routing_keys = jax.random.split(jax.random.fold_in(own_keys[1], 1), TOKENS // TOK_DEV)
    routing_turns = jax.random.permutation(jax.random.fold_in(own_keys[1], 3), TOKENS // TOK_DEV)
    routing = jax.vmap(lambda own, number: assign_block(jax.random.fold_in(own_keys[1], 2), own, number, TOK_DEV, EXPERTS, TOP, CAP, 2))(routing_keys, routing_turns).reshape((TOKENS, TOP))
    gates = jnp.clip(0.2 + 0.8 * jax.random.uniform(own_keys[2], (TOKENS, TOP), jnp.float32) ** levels(own_keys[2], (TOKENS, TOP), ((0, 16),), -0.2, 0.2), 0.2, 1.0)
    norm_gain = jnp.clip(1.0 + 0.18 * jax.random.normal(key_of[3], (D,), jnp.float32), 0.099609375, 1.8984375).astype(jnp.bfloat16)
    w_gate = normal_values(key_of[4], (N_EP, D, FF // GROUP), D ** -0.5, 0.125, ((0, 16),))
    w_up = normal_values(key_of[5], (N_EP, D, FF // GROUP), D ** -0.5, 0.125, ((0, 16),))
    w_down = normal_values(key_of[6], (N_EP, FF // GROUP, D), FF ** -0.5, 0.09375, ((0, 16),))
    return dict(tokens=tokens, routing=routing, gates=gates, norm_gain=norm_gain, w_gate=w_gate, w_up=w_up, w_down=w_down)


def run_expert(operands):
    expert_rows, gate_piece, up_piece, down_piece = operands
    gate_matrix = jnp.moveaxis(gate_piece, 0, 1).reshape(D, FF)
    up_matrix = jnp.moveaxis(up_piece, 0, 1).reshape(D, FF)
    gate_act = jnp.dot(expert_rows, gate_matrix, preferred_element_type=jnp.float32)
    up_act = jnp.dot(expert_rows, up_matrix, preferred_element_type=jnp.float32)
    hidden = (jax.nn.silu(gate_act) * up_act).astype(jnp.bfloat16)
    return jnp.dot(hidden, down_piece, preferred_element_type=jnp.float32).astype(jnp.bfloat16)

def reference(tokens, routing, gates, norm_gain, w_gate, w_up, w_down):
    values = tokens.astype(jnp.float32)
    scale = lax.rsqrt(lax.optimization_barrier(jnp.mean(values * values, axis=-1, keepdims=True)) + 1e-06)
    normed = (values * scale * norm_gain.astype(jnp.float32)).astype(jnp.bfloat16)
    blocks = routing.reshape(N_EP, TOK_DEV, TOP).astype(jnp.int32)
    one_hot = (blocks[..., None] == jnp.arange(EXPERTS, dtype=jnp.int32)).astype(jnp.int32)
    per_token = lax.optimization_barrier(jnp.sum(one_hot, axis=2)).astype(jnp.int32)
    before = (jnp.cumsum(per_token, axis=1) - per_token).astype(jnp.int32)
    slots = lax.optimization_barrier(jnp.sum(one_hot * before[:, :, None, :], axis=-1)).astype(jnp.int32)
    source = jnp.arange(N_EP, dtype=jnp.int32)[:, None, None]
    target = ((blocks * N_EP + source) * CAP + slots).reshape(-1).astype(jnp.int32)
    filled = jnp.zeros((EXPERTS * N_EP * CAP, D), jnp.bfloat16)
    filled = filled.at[target].set(jnp.repeat(normed, TOP, axis=0))
    expert_rows = filled.reshape(EXPERTS, N_EP * CAP, D)
    gate_pieces = w_gate.reshape(EXPERTS, GROUP, D, FF // GROUP)
    up_pieces = w_up.reshape(EXPERTS, GROUP, D, FF // GROUP)
    down_pieces = w_down.reshape(EXPERTS, FF, D)
    results = lax.map(run_expert, (expert_rows, gate_pieces, up_pieces, down_pieces))
    picked = results.reshape(EXPERTS * N_EP * CAP, D)[target].reshape(N_EP * TOK_DEV, TOP, D)
    mixed = lax.optimization_barrier(jnp.sum(gates[..., None] * picked.astype(jnp.float32), axis=1))
    return mixed.astype(jnp.bfloat16)
```

```python
import functools

import jax
import jax.numpy as jnp
from jax import lax
from jax.experimental import pallas as pl
from jax.experimental.pallas import tpu as pltpu
from jax.sharding import PartitionSpec as P

GROUP = 4
LANE = 128
PIECES = 4
PARTS = 2


def kernel(n, cap, tok_in, rt_in, gt_in, gain_in, wg, wu, wd, out_to,
           tok, rt, gt, gain, out, normed, outgoing, xbuf, wgu, wdn, hidden, part, give, take, cross, crossed,
           finished, ret, total, table, turned, code, in_sem, w_sem, out_sem,
           zs, zr, ys, yr, cs, cr, fs, fr, gs, gr, bs, br, es, er):
    toks, width = tok.shape
    ff = wg.shape[1]
    me = lax.axis_index("ep")
    g, j = me // GROUP, me % GROUP
    partner = g * GROUP + (j + 1 - 2 * (j % 2))
    across = g * GROUP + (j + 2) % GROUP
    span = width // PIECES
    half = width // PARTS

    upper = (2 * g) // n
    edge = g + upper * (n - 1 - 2 * g)
    inner = 1 - 2 * upper

    def source(i):
        past = jnp.minimum(1, i // (2 * edge + 1))
        far = (1 - past) * ((i + 1) // 2) + past * (i - edge)
        way = past + (1 - past) * (2 * (i % 2) - 1)
        return g + inner * way * far

    def remote(src, dst, send, recv, device):
        return pltpu.make_async_remote_copy(
            src_ref=src, dst_ref=dst, send_sem=send, recv_sem=recv,
            device_id={"ep": device}, device_id_type=pl.DeviceIdType.MESH)

    barrier = pltpu.get_barrier_semaphore()
    others = [partner, across] + [source(i) * GROUP + j for i in range(1, n)]
    for other in others:
        pl.semaphore_signal(barrier, inc=1, device_id={"ep": other},
                            device_id_type=pl.DeviceIdType.MESH)

    inputs = [pltpu.make_async_copy(a, b, in_sem.at[k])
              for k, (a, b) in enumerate([(tok_in, tok), (rt_in, rt), (gt_in, gt), (gain_in, gain)])]
    for copy in inputs:
        copy.start()
    tiles = ff // LANE
    loads = []
    for t in range(tiles):
        loads.append(pltpu.make_async_copy(wg.at[:, pl.ds(t * LANE, LANE)], wgu.at[t, :, pl.ds(0, LANE)], w_sem.at[2 * t]))
        loads.append(pltpu.make_async_copy(wu.at[:, pl.ds(t * LANE, LANE)], wgu.at[t, :, pl.ds(LANE, LANE)], w_sem.at[2 * t + 1]))
    loads.append(pltpu.make_async_copy(wd, wdn, w_sem.at[2 * tiles]))
    table[...] = jnp.zeros_like(table)
    for copy in inputs:
        copy.wait()
    for copy in loads:
        copy.start()

    values = tok[...].astype(jnp.float32)
    scale = lax.rsqrt(jnp.mean(values * values, axis=-1, keepdims=True) + 1e-06)
    normed[...] = (values * scale * gain[...].reshape(1, width).astype(jnp.float32)).astype(jnp.bfloat16)

    table[0:2] = rt[...].astype(jnp.float32)
    table[2:4] = gt[...]
    turned[...] = table[...].T
    experts_at = lax.broadcasted_iota(jnp.int32, (toks, LANE), 1).astype(jnp.float32)
    named = ((experts_at == turned[:, 0:1]) | (experts_at == turned[:, 1:2])).astype(jnp.float32)
    lower = (lax.broadcasted_iota(jnp.int32, (toks, toks), 1)
             < lax.broadcasted_iota(jnp.int32, (toks, toks), 0)).astype(jnp.bfloat16)
    before = jnp.dot(lower, named.astype(jnp.bfloat16), preferred_element_type=jnp.float32)
    code[...] = jnp.where(named > 0.5, before, -1.0)
    table[...] = code[...].T

    def pack(e, dst):
        row = jnp.sum(jnp.where(lax.broadcasted_iota(jnp.int32, (LANE, toks), 0) == e, table[...], 0.0), axis=0, keepdims=True)
        slot = lax.broadcasted_iota(jnp.int32, (cap, toks), 0).astype(jnp.float32)
        pick = (slot == row).astype(jnp.bfloat16)
        for t in range(width // 512):
            cols = pl.ds(t * 512, 512)
            dst[:, cols] = jnp.dot(pick, normed[:, cols], preferred_element_type=jnp.float32).astype(jnp.bfloat16)

    def lane_rows(lane, count=1):
        return pl.ds(pl.multiple_of(lane * cap, cap), count * cap)

    def part_of(p):
        return pl.ds(p * half, half)

    def piece_of(h):
        return pl.ds(h * span, span)

    def lane_copy(i, p, src, dst, send, recv, device):
        s = source(i)
        return remote(xbuf.at[s, lane_rows(src), part_of(p)], xbuf.at[s, lane_rows(dst), part_of(p)],
                      send.at[i, p], recv.at[i, p], device)

    def across_copy(i, p):
        return lane_copy(i, p, 0, 2, ys, yr, across)

    def beside_copy(i, p):
        return lane_copy(i, p, 0, 1, cs, cr, partner)

    def forward_copy(i, p):
        return lane_copy(i, p, 2, 3, fs, fr, partner)

    def source_copy(i, p, to, at):
        return remote(outgoing.at[i, :, part_of(p)], xbuf.at[at, lane_rows(0), part_of(p)],
                      zs.at[i, p], zr.at[at, p], to * GROUP + j)

    def give_copy(i, side, h):
        return remote(give.at[i, side, :, piece_of(h)], take.at[i, side, :, piece_of(h)],
                      gs.at[2 * i + side, h], gr.at[2 * i + side, h], partner)

    def cross_copy(i, h):
        return remote(cross.at[i, :, piece_of(h)], crossed.at[i, :, piece_of(h)],
                      bs.at[i, h], br.at[i, h], across)

    def return_copy(i, h, to, at):
        return remote(finished.at[i, :, piece_of(h)], ret.at[at, :, piece_of(h)],
                      es.at[i, h], er.at[at, h], to * GROUP + j)

    def depart(i):
        for p in range(PARTS):
            source_copy(i, p, source(i), g).start()

    def relay(i, p):
        source_copy(i, p, partner // GROUP, source(i)).wait_recv()
        across_copy(i, p).start()
        beside_copy(i, p).start()

    def forward(i, p):
        across_copy(i, p).wait_recv()
        forward_copy(i, p).start()

    def rise(i, side):
        rows = xbuf[source(i), lane_rows(2 * side, 2)]
        for t in range(tiles):
            both = jnp.dot(rows, wgu[t], preferred_element_type=jnp.float32)
            gate_act, up_act = both[:, :LANE], both[:, LANE:]
            act = gate_act / (1.0 + jnp.exp(-gate_act)) * up_act
            hidden[:, pl.ds(t * LANE, LANE)] = act.astype(jnp.bfloat16)

    def fall(i, side):
        for h in pieces:
            cols = piece_of(h)
            piece = jnp.dot(hidden[...], wdn[:, cols], preferred_element_type=jnp.float32)
            part[i, side, :, cols] = piece[0:cap]
            give[i, side, :, cols] = piece[cap:2 * cap].astype(jnp.bfloat16)
        for h in pieces:
            give_copy(i, side, h).start()

    def reduce_pair(i, h, send):
        give_copy(i, 1, h).wait_recv()
        cols = piece_of(h)
        cross[i, :, cols] = (part[i, 1, :, cols] + take[i, 1, :, cols].astype(jnp.float32)).astype(jnp.bfloat16)
        if send:
            cross_copy(i, h).start()

    def send_cross(i):
        for h in pieces:
            cross_copy(i, h).start()

    def finish(i, h):
        give_copy(i, 0, h).wait_recv()
        cross_copy(i, h).wait_recv()
        cols = piece_of(h)
        done = (part[i, 0, :, cols] + take[i, 0, :, cols].astype(jnp.float32)
                + crossed[i, :, cols].astype(jnp.float32)).astype(jnp.bfloat16)
        if i == 0:
            ret[g, :, cols] = done
        else:
            finished[i, :, cols] = done
            return_copy(i, h, source(i), g).start()

    def mixer(i):
        e = source(i)
        experts_at = lax.broadcasted_iota(jnp.int32, (toks, LANE), 1)
        column = jnp.sum(jnp.where(experts_at == e, code[...], 0.0), axis=1, keepdims=True)
        slot = lax.broadcasted_iota(jnp.int32, (toks, cap), 1).astype(jnp.float32)
        pick = (slot == column).astype(jnp.bfloat16)
        name = e.astype(jnp.float32)
        gate = (jnp.where(turned[:, 0:1] == name, turned[:, 2:3], 0.0)
                + jnp.where(turned[:, 1:2] == name, turned[:, 3:4], 0.0))
        def mix(h, start, last):
            cols = piece_of(h)
            if i:
                return_copy(i, h, partner // GROUP, e).wait_recv()
            term = gate * jnp.dot(pick, ret[e, :, cols], preferred_element_type=jnp.float32)
            if not start:
                term = total[:, cols] + term
            if last:
                out[:, cols] = term.astype(jnp.bfloat16)
                pltpu.make_async_copy(out.at[:, cols], out_to.at[:, cols], out_sem.at[h]).start()
            else:
                total[:, cols] = term

        return mix

    def mix_all(i, start, last):
        mix = mixer(i)
        for h in pieces:
            mix(h, start, last)

    def own(last):
        mix = mixer(0)
        for h in pieces:
            finish(0, h)
            mix(h, False, last)

    pieces = range(PIECES)
    parts = range(PARTS)
    at_edge, within = edge == 0, edge > 0
    pack(g, xbuf.at[g, lane_rows(0)])
    pack(source(1), outgoing.at[1])
    pl.semaphore_wait(barrier, len(others))
    for p in parts:
        across_copy(0, p).start()
        beside_copy(0, p).start()
    depart(1)
    for i in range(2, n):
        pack(source(i), outgoing.at[i])

        @pl.when(within)
        def _():
            depart(i)
    for load in loads:
        load.wait()

    def step(k, carry):
        def at(c):
            return pl.when(k == c)

        def when_is(c):
            return (k == c).astype(jnp.int32)

        i = k // 2 + when_is(1) - when_is(3)
        side = k % 2 + when_is(2) - when_is(1)

        @at(1)
        def _():
            for p in parts:
                forward(0, p)
                relay(1, p)

            @pl.when(within)
            def _():
                for p in parts:
                    relay(2, p)

        @at(2)
        def _():
            for p in parts:
                forward(1, p)

                @pl.when(at_edge)
                def _():
                    relay(2, p)

            @pl.when(at_edge)
            def _():
                for o in range(2, n):
                    depart(o)

        for o in range(3, n):
            @at(2 * o - 2)
            def _():
                @pl.when(within)
                def _():
                    relay(o, 0)

            @at(2 * o - 1)
            def _():
                for p in parts:
                    forward(o - 1, p)

                @pl.when(within)
                def _():
                    for p in parts[1:]:
                        relay(o, p)
                    if o == 3:
                        send_cross(1)

            @at(2 * o)
            def _():
                @pl.when(at_edge)
                def _():
                    for h in pieces[:-1]:
                        finish(o - 2, h)
                    relay(o, 0)
                    finish(o - 2, PIECES - 1)
                    for p in parts[1:]:
                        relay(o, p)
                if o < n - 1:
                    @pl.when(within)
                    def _():
                        for h in pieces:
                            finish(o - 2, h)

        @at(2 * n - 1)
        def _():
            for p in parts:
                forward(n - 1, p)

            @pl.when(within)
            def _():
                for h in pieces[:PIECES // 2]:
                    finish(n - 3, h)

        @pl.when(side == 0)
        def _():
            for p in parts:
                beside_copy(i, p).wait_recv()

        @pl.when(side == 1)
        def _():
            for p in parts:
                forward_copy(i, p).wait_recv()
        rise(i, side)

        @at(3)
        def _():
            for h in pieces:
                reduce_pair(1, h, False)

            @pl.when(at_edge)
            def _():
                send_cross(1)

        @at(4)
        def _():
            for h in pieces:
                reduce_pair(0, h, False)
        for o in range(3, n):
            @at(2 * o)
            def _():
                for h in pieces:
                    reduce_pair(o - 1, h, True)

        @at(2 * n - 1)
        def _():
            @pl.when(within)
            def _():
                for h in pieces[PIECES // 2:]:
                    finish(n - 3, h)
        fall(i, side)
        return carry

    lax.fori_loop(0, 2 * n, step, 0)
    for h in pieces[:PIECES // 2]:
        finish(n - 2, h)
    for h in pieces:
        reduce_pair(n - 1, h, True)
    send_cross(0)
    for h in pieces[PIECES // 2:]:
        finish(n - 2, h)
    for h in pieces:
        finish(n - 1, h)
    mix_all(1, True, False)

    @pl.when(at_edge)
    def _():
        own(False)
        for i in range(n - 1, 1, -1):
            mix_all(i, False, i == 2)

    @pl.when(within)
    def _():
        for i in range(2, n):
            mix_all(i, False, False)
        own(True)
    for h in pieces:
        pltpu.make_async_copy(out.at[:, piece_of(h)], out_to.at[:, piece_of(h)], out_sem.at[h]).wait()
    for i in range(n):
        for p in parts:
            across_copy(i, p).wait_send()
            beside_copy(i, p).wait_send()
            forward_copy(i, p).wait_send()
            if i:
                source_copy(i, p, source(i), g).wait_send()
        for h in pieces:
            give_copy(i, 0, h).wait_send()
            give_copy(i, 1, h).wait_send()
            cross_copy(i, h).wait_send()
            if i:
                return_copy(i, h, source(i), g).wait_send()


def per_device(tokens, routing, gates, norm_gain, w_gate, w_up, w_down):
    toks, width = tokens.shape
    top = routing.shape[1]
    devices = lax.axis_size("ep")
    n = devices // GROUP
    cap = GROUP * (5 * toks * top // (4 * devices))
    cap = -(-cap // 16) * 16
    ff = w_gate.shape[2]
    bf, f32 = jnp.bfloat16, jnp.float32
    by_part = pltpu.SemaphoreType.DMA((n, PARTS))
    by_side = pltpu.SemaphoreType.DMA((2 * n, PIECES))
    by_piece = pltpu.SemaphoreType.DMA((n, PIECES))
    hbm = pl.BlockSpec(memory_space=pl.ANY)
    return pl.pallas_call(
        functools.partial(kernel, n, cap),
        out_shape=jax.ShapeDtypeStruct((toks, width), bf),
        in_specs=[hbm] * 7,
        out_specs=hbm,
        scratch_shapes=[
            pltpu.VMEM((toks, width), bf),
            pltpu.VMEM((top, toks), jnp.int32),
            pltpu.VMEM((top, toks), f32),
            pltpu.VMEM((width,), bf),
            pltpu.VMEM((toks, width), bf),
            pltpu.VMEM((toks, width), bf),
            pltpu.VMEM((n, cap, width), bf),
            pltpu.VMEM((n, GROUP * cap, width), bf),
            pltpu.VMEM((ff // LANE, width, 2 * LANE), bf),
            pltpu.VMEM((ff, width), bf),
            pltpu.VMEM((2 * cap, ff), bf),
            pltpu.VMEM((n, 2, cap, width), f32),
            pltpu.VMEM((n, 2, cap, width), bf),
            pltpu.VMEM((n, 2, cap, width), bf),
            pltpu.VMEM((n, cap, width), bf),
            pltpu.VMEM((n, cap, width), bf),
            pltpu.VMEM((n, cap, width), bf),
            pltpu.VMEM((n, cap, width), bf),
            pltpu.VMEM((toks, width), f32),
            pltpu.VMEM((LANE, toks), f32),
            pltpu.VMEM((toks, LANE), f32),
            pltpu.VMEM((toks, LANE), f32),
            pltpu.SemaphoreType.DMA((4,)),
            pltpu.SemaphoreType.DMA((2 * (ff // LANE) + 1,)),
            pltpu.SemaphoreType.DMA((PIECES,)),
        ] + [by_part] * 8 + [by_side] * 2 + [by_piece] * 4,
        compiler_params=pltpu.CompilerParams(
            collective_id=0, has_side_effects=True, vmem_limit_bytes=62 * 1024 * 1024),
    )(tokens, routing.T, gates.T, norm_gain, w_gate.reshape(w_gate.shape[1:]),
      w_up.reshape(w_up.shape[1:]), w_down.reshape(w_down.shape[1:]))


def solution(mesh):
    placed = (
        P(("grp", "ep"), None),
        P(("grp", "ep"), None),
        P(("grp", "ep"), None),
        P(),
        P("ep", None, None),
        P("ep", None, None),
        P("ep", None, None),
    )
    return jax.shard_map(
        per_device, mesh=mesh, in_specs=placed, out_specs=P(("grp", "ep"), None), check_vma=False
    )
```

```python
import functools

import jax
import jax.numpy as jnp
from jax import lax
from jax.experimental import pallas as pl
from jax.experimental.pallas import tpu as pltpu
from jax.sharding import PartitionSpec as P

GROUP = 4
LANE = 128
PIECES = 4
PARTS = 2


def kernel(n, cap, tok_in, rt_in, gt_in, gain_in, wg, wu, wd, out_to,
           tok, rt, gt, gain, out, normed, outgoing, xbuf, wgu, wdn, hidden, part, give, take, cross, crossed,
           finished, ret, total, table, turned, code, in_sem, w_sem, out_sem,
           zs, zr, ys, yr, cs, cr, fs, fr, gs, gr, bs, br, es, er):
    toks, width = tok.shape
    ff = wg.shape[1]
    me = lax.axis_index("ep")
    g, j = me // GROUP, me % GROUP
    partner = g * GROUP + (j + 1 - 2 * (j % 2))
    across = g * GROUP + (j + 2) % GROUP
    span = width // PIECES
    half = width // PARTS

    upper = (2 * g) // n
    edge = g + upper * (n - 1 - 2 * g)
    inner = 1 - 2 * upper

    def source(i):
        past = jnp.minimum(1, i // (2 * edge + 1))
        far = (1 - past) * ((i + 1) // 2) + past * (i - edge)
        way = past + (1 - past) * (2 * (i % 2) - 1)
        return g + inner * way * far

    def remote(src, dst, send, recv, device):
        return pltpu.make_async_remote_copy(
            src_ref=src, dst_ref=dst, send_sem=send, recv_sem=recv,
            device_id={"ep": device}, device_id_type=pl.DeviceIdType.MESH)

    barrier = pltpu.get_barrier_semaphore()
    others = [partner, across] + [source(i) * GROUP + j for i in range(1, n)]
    for other in others:
        pl.semaphore_signal(barrier, inc=1, device_id={"ep": other},
                            device_id_type=pl.DeviceIdType.MESH)

    inputs = [pltpu.make_async_copy(a, b, in_sem.at[k])
              for k, (a, b) in enumerate([(tok_in, tok), (gain_in, gain), (rt_in, rt), (gt_in, gt)])]
    for copy in inputs:
        copy.start()
    tiles = ff // LANE
    loads = []
    for t in range(tiles):
        loads.append(pltpu.make_async_copy(wg.at[:, pl.ds(t * LANE, LANE)], wgu.at[t, :, pl.ds(0, LANE)], w_sem.at[2 * t]))
        loads.append(pltpu.make_async_copy(wu.at[:, pl.ds(t * LANE, LANE)], wgu.at[t, :, pl.ds(LANE, LANE)], w_sem.at[2 * t + 1]))
    loads.append(pltpu.make_async_copy(wd, wdn, w_sem.at[2 * tiles]))
    table[...] = jnp.zeros_like(table)
    for copy in inputs[2:]:
        copy.wait()
    table[0:2] = rt[...].astype(jnp.float32)
    table[2:4] = gt[...]
    turned[...] = table[...].T
    experts_at = lax.broadcasted_iota(jnp.int32, (toks, LANE), 1).astype(jnp.float32)
    named = ((experts_at == turned[:, 0:1]) | (experts_at == turned[:, 1:2])).astype(jnp.float32)
    lower = (lax.broadcasted_iota(jnp.int32, (toks, toks), 1)
             < lax.broadcasted_iota(jnp.int32, (toks, toks), 0)).astype(jnp.bfloat16)
    before = jnp.dot(lower, named.astype(jnp.bfloat16), preferred_element_type=jnp.float32)
    code[...] = jnp.where(named > 0.5, before, -1.0)
    table[...] = code[...].T

    for copy in inputs[:2]:
        copy.wait()
    for copy in loads:
        copy.start()
    values = tok[...].astype(jnp.float32)
    scale = lax.rsqrt(jnp.mean(values * values, axis=-1, keepdims=True) + 1e-06)
    normed[...] = (values * scale * gain[...].reshape(1, width).astype(jnp.float32)).astype(jnp.bfloat16)

    def pack(e, dst):
        row = jnp.sum(jnp.where(lax.broadcasted_iota(jnp.int32, (LANE, toks), 0) == e, table[...], 0.0), axis=0, keepdims=True)
        slot = lax.broadcasted_iota(jnp.int32, (cap, toks), 0).astype(jnp.float32)
        pick = (slot == row).astype(jnp.bfloat16)
        for t in range(width // 512):
            cols = pl.ds(t * 512, 512)
            dst[:, cols] = jnp.dot(pick, normed[:, cols], preferred_element_type=jnp.float32).astype(jnp.bfloat16)

    def lane_rows(lane, count=1):
        return pl.ds(pl.multiple_of(lane * cap, cap), count * cap)

    def part_of(p):
        return pl.ds(p * half, half)

    def piece_of(h):
        return pl.ds(h * span, span)

    def lane_copy(i, p, src, dst, send, recv, device):
        s = source(i)
        return remote(xbuf.at[s, lane_rows(src), part_of(p)], xbuf.at[s, lane_rows(dst), part_of(p)],
                      send.at[i, p], recv.at[i, p], device)

    def across_copy(i, p):
        return lane_copy(i, p, 0, 2, ys, yr, across)

    def beside_copy(i, p):
        return lane_copy(i, p, 0, 1, cs, cr, partner)

    def forward_copy(i, p):
        return lane_copy(i, p, 2, 3, fs, fr, partner)

    def source_copy(i, p, to, at):
        return remote(outgoing.at[i, :, part_of(p)], xbuf.at[at, lane_rows(0), part_of(p)],
                      zs.at[i, p], zr.at[at, p], to * GROUP + j)

    def give_copy(i, side, h):
        return remote(give.at[i, side, :, piece_of(h)], take.at[i, side, :, piece_of(h)],
                      gs.at[2 * i + side, h], gr.at[2 * i + side, h], partner)

    def cross_copy(i, h):
        return remote(cross.at[i, :, piece_of(h)], crossed.at[i, :, piece_of(h)],
                      bs.at[i, h], br.at[i, h], across)

    def return_copy(i, h, to, at):
        return remote(finished.at[i, :, piece_of(h)], ret.at[at, :, piece_of(h)],
                      es.at[i, h], er.at[at, h], to * GROUP + j)

    def depart(i):
        for p in range(PARTS):
            source_copy(i, p, source(i), g).start()

    def relay(i, p):
        source_copy(i, p, partner // GROUP, source(i)).wait_recv()
        across_copy(i, p).start()
        beside_copy(i, p).start()

    def forward(i, p):
        across_copy(i, p).wait_recv()
        forward_copy(i, p).start()

    def rise(i, side):
        rows = xbuf[source(i), lane_rows(2 * side, 2)]
        for t in range(tiles):
            both = jnp.dot(rows, wgu[t], preferred_element_type=jnp.float32)
            gate_act, up_act = both[:, :LANE], both[:, LANE:]
            act = gate_act / (1.0 + jnp.exp(-gate_act)) * up_act
            hidden[:, pl.ds(t * LANE, LANE)] = act.astype(jnp.bfloat16)

    def fall(i, side):
        for h in pieces:
            cols = piece_of(h)
            piece = jnp.dot(hidden[...], wdn[:, cols], preferred_element_type=jnp.float32)
            part[i, side, :, cols] = piece[0:cap]
            give[i, side, :, cols] = piece[cap:2 * cap].astype(jnp.bfloat16)
        for h in pieces:
            give_copy(i, side, h).start()

    def reduce_pair(i, h, send):
        give_copy(i, 1, h).wait_recv()
        cols = piece_of(h)
        cross[i, :, cols] = (part[i, 1, :, cols] + take[i, 1, :, cols].astype(jnp.float32)).astype(jnp.bfloat16)
        if send:
            cross_copy(i, h).start()

    def send_cross(i):
        for h in pieces:
            cross_copy(i, h).start()

    def finish(i, h):
        give_copy(i, 0, h).wait_recv()
        cross_copy(i, h).wait_recv()
        cols = piece_of(h)
        done = (part[i, 0, :, cols] + take[i, 0, :, cols].astype(jnp.float32)
                + crossed[i, :, cols].astype(jnp.float32)).astype(jnp.bfloat16)
        if i == 0:
            ret[g, :, cols] = done
        else:
            finished[i, :, cols] = done
            return_copy(i, h, source(i), g).start()

    def returned(i, h):
        return_copy(i, h, partner // GROUP, source(i)).wait_recv()

    def mixer(i):
        e = source(i)
        experts_at = lax.broadcasted_iota(jnp.int32, (toks, LANE), 1)
        column = jnp.sum(jnp.where(experts_at == e, code[...], 0.0), axis=1, keepdims=True)
        slot = lax.broadcasted_iota(jnp.int32, (toks, cap), 1).astype(jnp.float32)
        pick = (slot == column).astype(jnp.bfloat16)
        name = e.astype(jnp.float32)
        gate = (jnp.where(turned[:, 0:1] == name, turned[:, 2:3], 0.0)
                + jnp.where(turned[:, 1:2] == name, turned[:, 3:4], 0.0))
        def mix(h, start, last):
            cols = piece_of(h)
            if i:
                returned(i, h)
            term = gate * jnp.dot(pick, ret[e, :, cols], preferred_element_type=jnp.float32)
            if not start:
                term = total[:, cols] + term
            if last:
                out[:, cols] = term.astype(jnp.bfloat16)
                pltpu.make_async_copy(out.at[:, cols], out_to.at[:, cols], out_sem.at[h]).start()
            else:
                total[:, cols] = term

        return mix

    def mix_all(i, start, last):
        mix = mixer(i)
        for h in pieces:
            mix(h, start, last)

    def own(start, last):
        mix = mixer(0)
        for h in pieces:
            finish(0, h)
            mix(h, start, last)

    pieces = range(PIECES)
    parts = range(PARTS)
    at_edge, within = edge == 0, edge > 0
    pack(g, xbuf.at[g, lane_rows(0)])
    pack(source(1), outgoing.at[1])
    pl.semaphore_wait(barrier, len(others))
    for p in parts:
        across_copy(0, p).start()
        beside_copy(0, p).start()
    depart(1)
    for i in range(2, n):
        pack(source(i), outgoing.at[i])

        @pl.when(within)
        def _():
            depart(i)
    for load in loads:
        load.wait()

    def step(k, carry):
        def at(c):
            return pl.when(k == c)

        def when_is(c):
            return (k == c).astype(jnp.int32)

        i = k // 2 + when_is(1) + when_is(3) - 2 * when_is(5)
        side = k % 2 + when_is(2) + when_is(4) - when_is(1) - when_is(3)

        @at(1)
        def _():
            for p in parts:
                forward(0, p)
                relay(1, p)

            @pl.when(within)
            def _():
                for p in parts:
                    relay(2, p)

        @at(2)
        def _():
            for p in parts:
                forward(1, p)

                @pl.when(at_edge)
                def _():
                    relay(2, p)
                    if p == 0:
                        for o in range(2, n):
                            depart(o)

        @at(4)
        def _():
            for p in parts:
                forward(2, p)

        for o in range(3, n):
            @at(2 * o - 1)
            def _():
                if o > 3:
                    for p in parts:
                        forward(o - 1, p)

                @pl.when(within)
                def _():
                    for p in parts:
                        relay(o, p)

            @at(2 * o)
            def _():
                for h in pieces[:-1]:
                    finish(o - 2, h)

                @pl.when(at_edge)
                def _():
                    relay(o, 0)
                finish(o - 2, PIECES - 1)

                @pl.when(at_edge)
                def _():
                    for p in parts[1:]:
                        relay(o, p)

        @at(2 * n - 1)
        def _():
            @pl.when(at_edge)
            def _():
                send_cross(0)
                for h in pieces:
                    finish(n - 2, h)
            for p in parts:
                forward(n - 1, p)

        @pl.when(side == 0)
        def _():
            for p in parts:
                beside_copy(i, p).wait_recv()

        @pl.when(side == 1)
        def _():
            for p in parts:
                forward_copy(i, p).wait_recv()
        rise(i, side)

        @at(2 * n - 1)
        def _():
            @pl.when(within)
            def _():
                finish(n - 2, 0)
        for o in range(n - 1):
            @at(6 if o == 0 else 3 if o == 1 else 5 if o == 2 else 2 * o + 2)
            def _():
                for h in pieces:
                    reduce_pair(o, h, o > 0)
        fall(i, side)
        return carry

    lax.fori_loop(0, 2 * n, step, 0)
    @pl.when(at_edge)
    def _():
        for h in pieces:
            reduce_pair(n - 1, h, True)
        own(True, False)
        for h in pieces:
            finish(n - 1, h)
        mixers = [mixer(i) for i in range(1, n)]
        for h in pieces:
            for mix in mixers:
                mix(h, False, mix is mixers[-1])

    @pl.when(within)
    def _():
        finish(n - 2, 1)
        for h in pieces:
            reduce_pair(n - 1, h, True)
        send_cross(0)
        for h in pieces[2:]:
            finish(n - 2, h)
        for h in pieces:
            finish(n - 1, h)
        for i in range(1, n):
            mix_all(i, i == 1, False)
        own(False, True)
    for h in pieces:
        pltpu.make_async_copy(out.at[:, piece_of(h)], out_to.at[:, piece_of(h)], out_sem.at[h]).wait()
    for i in range(n):
        for p in parts:
            across_copy(i, p).wait_send()
            beside_copy(i, p).wait_send()
            forward_copy(i, p).wait_send()
            if i:
                source_copy(i, p, source(i), g).wait_send()
        for h in pieces:
            give_copy(i, 0, h).wait_send()
            give_copy(i, 1, h).wait_send()
            cross_copy(i, h).wait_send()
            if i:
                return_copy(i, h, source(i), g).wait_send()


def per_device(tokens, routing, gates, norm_gain, w_gate, w_up, w_down):
    toks, width = tokens.shape
    top = routing.shape[1]
    devices = lax.axis_size("ep")
    n = devices // GROUP
    cap = GROUP * (5 * toks * top // (4 * devices))
    cap = -(-cap // 16) * 16
    ff = w_gate.shape[2]
    bf, f32 = jnp.bfloat16, jnp.float32
    by_part = pltpu.SemaphoreType.DMA((n, PARTS))
    by_side = pltpu.SemaphoreType.DMA((2 * n, PIECES))
    by_piece = pltpu.SemaphoreType.DMA((n, PIECES))
    hbm = pl.BlockSpec(memory_space=pl.ANY)
    return pl.pallas_call(
        functools.partial(kernel, n, cap),
        out_shape=jax.ShapeDtypeStruct((toks, width), bf),
        in_specs=[hbm] * 7,
        out_specs=hbm,
        scratch_shapes=[
            pltpu.VMEM((toks, width), bf),
            pltpu.VMEM((top, toks), jnp.int32),
            pltpu.VMEM((top, toks), f32),
            pltpu.VMEM((width,), bf),
            pltpu.VMEM((toks, width), bf),
            pltpu.VMEM((toks, width), bf),
            pltpu.VMEM((n, cap, width), bf),
            pltpu.VMEM((n, GROUP * cap, width), bf),
            pltpu.VMEM((ff // LANE, width, 2 * LANE), bf),
            pltpu.VMEM((ff, width), bf),
            pltpu.VMEM((2 * cap, ff), bf),
            pltpu.VMEM((n, 2, cap, width), f32),
            pltpu.VMEM((n, 2, cap, width), bf),
            pltpu.VMEM((n, 2, cap, width), bf),
            pltpu.VMEM((n, cap, width), bf),
            pltpu.VMEM((n, cap, width), bf),
            pltpu.VMEM((n, cap, width), bf),
            pltpu.VMEM((n, cap, width), bf),
            pltpu.VMEM((toks, width), f32),
            pltpu.VMEM((LANE, toks), f32),
            pltpu.VMEM((toks, LANE), f32),
            pltpu.VMEM((toks, LANE), f32),
            pltpu.SemaphoreType.DMA((4,)),
            pltpu.SemaphoreType.DMA((2 * (ff // LANE) + 1,)),
            pltpu.SemaphoreType.DMA((PIECES,)),
        ] + [by_part] * 8 + [by_side] * 2 + [by_piece] * 4,
        compiler_params=pltpu.CompilerParams(
            collective_id=0, has_side_effects=True, vmem_limit_bytes=62 * 1024 * 1024),
    )(tokens, routing.T, gates.T, norm_gain, w_gate.reshape(w_gate.shape[1:]),
      w_up.reshape(w_up.shape[1:]), w_down.reshape(w_down.shape[1:]))


def solution(mesh):
    placed = (
        P(("grp", "ep"), None),
        P(("grp", "ep"), None),
        P(("grp", "ep"), None),
        P(),
        P("ep", None, None),
        P("ep", None, None),
        P("ep", None, None),
    )
    return jax.shard_map(
        per_device, mesh=mesh, in_specs=placed, out_specs=P(("grp", "ep"), None), check_vma=False
    )
```

```python
import functools

import jax
import jax.numpy as jnp
from jax import lax
from jax.experimental import pallas as pl
from jax.experimental.pallas import tpu as pltpu
from jax.sharding import PartitionSpec as P

GROUP = 4
LANE = 128
PIECES = 4
PARTS = 2


def kernel(n, cap, tok_in, rt_in, gt_in, gain_in, wg, wu, wd, out_to,
           tok, rt, gt, gain, out, normed, outgoing, xbuf, wgu, wdn, hidden, part, give, take, cross, crossed,
           finished, ret, total, table, turned, code, in_sem, w_sem, out_sem,
           sent, zr, yr, cr, fr, lr, gr, br, er):
    toks, width = tok.shape
    ff = wg.shape[1]
    me = lax.axis_index("ep")
    g, j = me // GROUP, me % GROUP
    partner = g * GROUP + (j + 1 - 2 * (j % 2))
    across = g * GROUP + (j + 2) % GROUP
    span = width // PIECES
    half = width // PARTS

    upper = (2 * g) // n
    edge = g + upper * (n - 1 - 2 * g)
    inner = 1 - 2 * upper

    def source(i):
        past = jnp.minimum(1, i // (2 * edge + 1))
        far = (1 - past) * ((i + 1) // 2) + past * (i - edge)
        way = past + (1 - past) * (2 * (i % 2) - 1)
        return g + inner * way * far

    def remote(src, dst, send, recv, device):
        return pltpu.make_async_remote_copy(
            src_ref=src, dst_ref=dst, send_sem=send, recv_sem=recv,
            device_id={"ep": device}, device_id_type=pl.DeviceIdType.MESH)

    barrier = pltpu.get_barrier_semaphore()
    others = [partner, across] + [source(i) * GROUP + j for i in range(1, n)]
    for other in others:
        pl.semaphore_signal(barrier, inc=1, device_id={"ep": other},
                            device_id_type=pl.DeviceIdType.MESH)

    inputs = [pltpu.make_async_copy(a, b, in_sem.at[k])
              for k, (a, b) in enumerate([(tok_in, tok), (gain_in, gain), (rt_in, rt), (gt_in, gt)])]
    for copy in inputs:
        copy.start()
    tiles = ff // LANE
    loads = []
    for t in range(tiles):
        loads.append(pltpu.make_async_copy(wg.at[:, pl.ds(t * LANE, LANE)], wgu.at[t, :, pl.ds(0, LANE)], w_sem.at[0]))
        loads.append(pltpu.make_async_copy(wu.at[:, pl.ds(t * LANE, LANE)], wgu.at[t, :, pl.ds(LANE, LANE)], w_sem.at[0]))
    loads.append(pltpu.make_async_copy(wd, wdn, w_sem.at[1]))
    table[...] = jnp.zeros_like(table)
    for copy in inputs[2:]:
        copy.wait()
    table[0:2] = rt[...].astype(jnp.float32)
    table[2:4] = gt[...]
    turned[...] = table[...].T
    experts_at = lax.broadcasted_iota(jnp.int32, (toks, LANE), 1).astype(jnp.float32)
    named = ((experts_at == turned[:, 0:1]) | (experts_at == turned[:, 1:2])).astype(jnp.float32)
    lower = (lax.broadcasted_iota(jnp.int32, (toks, toks), 1)
             < lax.broadcasted_iota(jnp.int32, (toks, toks), 0)).astype(jnp.bfloat16)
    before = jnp.dot(lower, named.astype(jnp.bfloat16), preferred_element_type=jnp.float32)
    code[...] = jnp.where(named > 0.5, before, -1.0)
    table[...] = code[...].T

    for copy in inputs[:2]:
        copy.wait()
    for copy in loads:
        copy.start()
    values = tok[...].astype(jnp.float32)
    scale = lax.rsqrt(jnp.mean(values * values, axis=-1, keepdims=True) + 1e-06)
    normed[...] = (values * scale * gain[...].reshape(1, width).astype(jnp.float32)).astype(jnp.bfloat16)

    def pack(e, dst):
        row = jnp.sum(jnp.where(lax.broadcasted_iota(jnp.int32, (LANE, toks), 0) == e, table[...], 0.0), axis=0, keepdims=True)
        slot = lax.broadcasted_iota(jnp.int32, (cap, toks), 0).astype(jnp.float32)
        pick = (slot == row).astype(jnp.bfloat16)
        for t in range(width // 512):
            cols = pl.ds(t * 512, 512)
            dst[:, cols] = jnp.dot(pick, normed[:, cols], preferred_element_type=jnp.float32).astype(jnp.bfloat16)

    def lane_rows(lane, count=1):
        return pl.ds(pl.multiple_of(lane * cap, cap), count * cap)

    def part_of(p):
        return pl.ds(p * half, half)

    def piece_of(h):
        return pl.ds(h * span, span)

    whole = pl.ds(0, width)

    def lane_copy(i, cols, src, dst, send, recv, device):
        s = source(i)
        return remote(xbuf.at[s, lane_rows(src), cols], xbuf.at[s, lane_rows(dst), cols], send, recv, device)

    def across_copy(i, p):
        return lane_copy(i, part_of(p), 0, 2, sent.at[0], yr.at[i, p], across)

    def beside_copy(i, cols):
        return lane_copy(i, cols, 0, 1, sent.at[1], cr.at[i], partner)

    def forward_copy(i, cols):
        return lane_copy(i, cols, 2, 3, sent.at[2], fr.at[i], partner)

    def source_copy(i, p, to, at):
        return remote(outgoing.at[i, :, part_of(p)], xbuf.at[at, lane_rows(0), part_of(p)],
                      sent.at[3], zr.at[at, p], to * GROUP + j)

    def low_give(i, cols):
        return remote(give.at[i, 0, :, cols], take.at[i, 0, :, cols], sent.at[4], lr.at[i], partner)

    def high_give(i, p):
        return remote(give.at[i, 1, :, part_of(p)], take.at[i, 1, :, part_of(p)], sent.at[4], gr.at[i, p], partner)

    def cross_copy(i, h):
        return remote(cross.at[i, :, piece_of(h)], crossed.at[i, :, piece_of(h)],
                      sent.at[5], br.at[i, h], across)

    def return_copy(i, h, to, at):
        return remote(finished.at[i, :, piece_of(h)], ret.at[at, :, piece_of(h)],
                      sent.at[7 if i == n - 1 else 6], er.at[at, h], to * GROUP + j)

    def depart(i):
        for p in range(PARTS):
            source_copy(i, p, source(i), g).start()

    def relay(i, p):
        source_copy(i, p, partner // GROUP, source(i)).wait_recv()
        across_copy(i, p).start()
        beside_copy(i, part_of(p)).start()

    def forward(i, p):
        across_copy(i, p).wait_recv()
        forward_copy(i, part_of(p)).start()

    def rise(i, side):
        rows = xbuf[source(i), lane_rows(2 * side, 2)]
        for t in range(tiles):
            both = jnp.dot(rows, wgu[t], preferred_element_type=jnp.float32)
            gate_act, up_act = both[:, :LANE], both[:, LANE:]
            act = gate_act / (1.0 + jnp.exp(-gate_act)) * up_act
            hidden[:, pl.ds(t * LANE, LANE)] = act.astype(jnp.bfloat16)

    def fall(i, side):
        for p in parts:
            for h in groups[p]:
                cols = piece_of(h)
                piece = jnp.dot(hidden[...], wdn[:, cols], preferred_element_type=jnp.float32)
                part[i, side, :, cols] = piece[0:cap]
                give[i, side, :, cols] = piece[cap:2 * cap].astype(jnp.bfloat16)

            @pl.when(side == 0)
            def _():
                low_give(i, part_of(p)).start()

            @pl.when(side == 1)
            def _():
                high_give(i, p).start()

    def reduce_pair(i, h, send):
        for p in parts:
            if h == groups[p][0]:
                high_give(i, p).wait_recv()
        cols = piece_of(h)
        cross[i, :, cols] = (part[i, 1, :, cols] + take[i, 1, :, cols].astype(jnp.float32)).astype(jnp.bfloat16)
        if send:
            cross_copy(i, h).start()

    def send_cross(i):
        for h in pieces:
            cross_copy(i, h).start()

    def finish(i, h):
        if h == 0:
            low_give(i, whole).wait_recv()
        cross_copy(i, h).wait_recv()
        cols = piece_of(h)
        done = (part[i, 0, :, cols] + take[i, 0, :, cols].astype(jnp.float32)
                + crossed[i, :, cols].astype(jnp.float32)).astype(jnp.bfloat16)
        if i == 0:
            ret[g, :, cols] = done
        else:
            finished[i, :, cols] = done
            return_copy(i, h, source(i), g).start()

    def returned(i, h):
        return_copy(i, h, partner // GROUP, source(i)).wait_recv()

    def mixer(i):
        e = source(i)
        experts_at = lax.broadcasted_iota(jnp.int32, (toks, LANE), 1)
        column = jnp.sum(jnp.where(experts_at == e, code[...], 0.0), axis=1, keepdims=True)
        slot = lax.broadcasted_iota(jnp.int32, (toks, cap), 1).astype(jnp.float32)
        pick = (slot == column).astype(jnp.bfloat16)
        name = e.astype(jnp.float32)
        gate = (jnp.where(turned[:, 0:1] == name, turned[:, 2:3], 0.0)
                + jnp.where(turned[:, 1:2] == name, turned[:, 3:4], 0.0))
        def mix(h, start, last):
            cols = piece_of(h)
            if i:
                returned(i, h)
            term = gate * jnp.dot(pick, ret[e, :, cols], preferred_element_type=jnp.float32)
            if not start:
                term = total[:, cols] + term
            if last:
                out[:, cols] = term.astype(jnp.bfloat16)
                pltpu.make_async_copy(out.at[:, cols], out_to.at[:, cols], out_sem.at[0]).start()
            else:
                total[:, cols] = term

        return mix

    def mix_all(i, start, last):
        mix = mixer(i)
        for h in pieces:
            mix(h, start, last)

    def own(start, last):
        mix = mixer(0)
        for h in pieces:
            finish(0, h)
            mix(h, start, last)

    pieces = range(PIECES)
    parts = range(PARTS)
    groups = [pieces[p * PIECES // PARTS:(p + 1) * PIECES // PARTS] for p in parts]
    at_edge, within = edge == 0, edge > 0
    pack(g, xbuf.at[g, lane_rows(0)])
    pl.semaphore_wait(barrier, len(others))
    for p in parts:
        across_copy(0, p).start()
        beside_copy(0, part_of(p)).start()
    pack(source(1), outgoing.at[1])
    depart(1)
    for i in range(2, n):
        pack(source(i), outgoing.at[i])

        @pl.when(within)
        def _():
            depart(i)
    pltpu.make_async_copy(wgu, wgu, w_sem.at[0]).wait()
    loads[-1].wait()

    def step(k, carry):
        def at(c):
            return pl.when(k == c)

        def when_is(c):
            return (k == c).astype(jnp.int32)

        i = k // 2 + when_is(1) + when_is(3) - 2 * when_is(5)
        side = k % 2 + when_is(2) + when_is(4) - when_is(1) - when_is(3)

        @at(1)
        def _():
            for p in parts:
                forward(0, p)
                relay(1, p)

            @pl.when(within)
            def _():
                for p in parts:
                    relay(2, p)

        @at(2)
        def _():
            for p in parts:
                forward(1, p)

                @pl.when(at_edge)
                def _():
                    relay(2, p)
                    if p == 0:
                        for o in range(2, n):
                            depart(o)

        @at(4)
        def _():
            for p in parts:
                forward(2, p)

        for o in range(3, n):
            @at(2 * o - 1)
            def _():
                if o > 3:
                    for p in parts:
                        forward(o - 1, p)

                if o > 3:
                    @pl.when(within)
                    def _():
                        for p in parts:
                            relay(o, p)

            @at(2 * o)
            def _():
                for h in pieces[:-1]:
                    finish(o - 2, h)

                @pl.when(at_edge)
                def _():
                    relay(o, 0)
                finish(o - 2, PIECES - 1)

                @pl.when(at_edge)
                def _():
                    for p in parts[1:]:
                        relay(o, p)

        @at(2 * n - 1)
        def _():
            @pl.when(at_edge)
            def _():
                send_cross(0)
                for h in pieces:
                    finish(n - 2, h)
            for p in parts:
                forward(n - 1, p)

        @pl.when(side == 0)
        def _():
            beside_copy(i, whole).wait_recv()

        @pl.when(side == 1)
        def _():
            forward_copy(i, whole).wait_recv()
        rise(i, side)

        @at(2 * n - 1)
        def _():
            @pl.when(within)
            def _():
                finish(n - 2, 0)
        for o in range(n - 1):
            @at(6 if o == 0 else 3 if o == 1 else 5 if o == 2 else 2 * o + 2)
            def _():
                for h in pieces[len(groups[0]):] if 0 < o < 3 else pieces:
                    reduce_pair(o, h, o > 0)
        fall(i, side)
        for o in (1, 2):
            @at(2 * o)
            def _():
                if o == 2:
                    @pl.when(within)
                    def _():
                        for p in parts:
                            relay(3, p)
                for h in groups[0]:
                    reduce_pair(o, h, True)
        return carry

    lax.fori_loop(0, 2 * n, step, 0)
    def drain():
        lane = [xbuf.at[:, lane_rows(k)] for k in range(3)]
        left = pl.ds(1, n - 1)
        for k, (src, dst) in enumerate([
                (lane[0], lane[2]), (lane[0], lane[1]), (lane[2], lane[1]),
                (outgoing.at[left], outgoing.at[left]), (give, take), (cross, crossed),
                (finished.at[pl.ds(1, n - 2)], ret.at[pl.ds(1, n - 2)])]):
            remote(src, dst, sent.at[k], yr.at[0, 0], partner).wait_send()

    @pl.when(at_edge)
    def _():
        for h in pieces:
            reduce_pair(n - 1, h, True)
        own(True, False)
        for h in pieces:
            finish(n - 1, h)
        drain()
        mixers = [mixer(i) for i in range(1, n)]
        for h in pieces:
            for mix in mixers:
                mix(h, False, mix is mixers[-1])

    @pl.when(within)
    def _():
        finish(n - 2, 1)
        for h in pieces:
            reduce_pair(n - 1, h, True)
        send_cross(0)
        for h in pieces[2:]:
            finish(n - 2, h)
        for h in pieces:
            finish(n - 1, h)
        for i in range(1, n):
            mix_all(i, i == 1, False)
        own(False, True)
        drain()
    remote(finished.at[n - 1], ret.at[0], sent.at[7], er.at[0, 0], partner).wait_send()
    pltpu.make_async_copy(out, out_to, out_sem.at[0]).wait()


def per_device(tokens, routing, gates, norm_gain, w_gate, w_up, w_down):
    toks, width = tokens.shape
    top = routing.shape[1]
    devices = lax.axis_size("ep")
    n = devices // GROUP
    cap = GROUP * (5 * toks * top // (4 * devices))
    cap = -(-cap // 16) * 16
    ff = w_gate.shape[2]
    bf, f32 = jnp.bfloat16, jnp.float32
    dma = pltpu.SemaphoreType.DMA
    hbm = pl.BlockSpec(memory_space=pl.ANY)
    return pl.pallas_call(
        functools.partial(kernel, n, cap),
        out_shape=jax.ShapeDtypeStruct((toks, width), bf),
        in_specs=[hbm] * 7,
        out_specs=hbm,
        scratch_shapes=[
            pltpu.VMEM((toks, width), bf),
            pltpu.VMEM((top, toks), jnp.int32),
            pltpu.VMEM((top, toks), f32),
            pltpu.VMEM((width,), bf),
            pltpu.VMEM((toks, width), bf),
            pltpu.VMEM((toks, width), bf),
            pltpu.VMEM((n, cap, width), bf),
            pltpu.VMEM((n, GROUP * cap, width), bf),
            pltpu.VMEM((ff // LANE, width, 2 * LANE), bf),
            pltpu.VMEM((ff, width), bf),
            pltpu.VMEM((2 * cap, ff), bf),
            pltpu.VMEM((n, 2, cap, width), f32),
            pltpu.VMEM((n, 2, cap, width), bf),
            pltpu.VMEM((n, 2, cap, width), bf),
            pltpu.VMEM((n, cap, width), bf),
            pltpu.VMEM((n, cap, width), bf),
            pltpu.VMEM((n, cap, width), bf),
            pltpu.VMEM((n, cap, width), bf),
            pltpu.VMEM((toks, width), f32),
            pltpu.VMEM((LANE, toks), f32),
            pltpu.VMEM((toks, LANE), f32),
            pltpu.VMEM((toks, LANE), f32),
            dma((4,)), dma((2,)), dma((1,)), dma((8,)), dma((n, PARTS)), dma((n, PARTS)), dma((n,)), dma((n,)),
            dma((n,)), dma((n, PARTS)), dma((n, PIECES)), dma((n, PIECES)),
        ],
        compiler_params=pltpu.CompilerParams(
            collective_id=0, has_side_effects=True, vmem_limit_bytes=62 * 1024 * 1024),
    )(tokens, routing.T, gates.T, norm_gain, w_gate.reshape(w_gate.shape[1:]),
      w_up.reshape(w_up.shape[1:]), w_down.reshape(w_down.shape[1:]))


def solution(mesh):
    placed = (
        P(("grp", "ep"), None),
        P(("grp", "ep"), None),
        P(("grp", "ep"), None),
        P(),
        P("ep", None, None),
        P("ep", None, None),
        P("ep", None, None),
    )
    return jax.shard_map(
        per_device, mesh=mesh, in_specs=placed, out_specs=P(("grp", "ep"), None), check_vma=False
    )
```

```python
import functools

import jax
import jax.numpy as jnp
from jax import lax
from jax.experimental import pallas as pl
from jax.experimental.pallas import tpu as pltpu
from jax.sharding import PartitionSpec as P

GROUP = 4
LANE = 128
PIECES = 4
PARTS = 2


def kernel(n, cap, tok_in, rt_in, gt_in, gain_in, wg, wu, wd, out_to,
           tok, rt, gt, gain, out, normed, outgoing, xbuf, wgu, wdn, hidden, part, give, take, cross, crossed,
           finished, ret, total, table, turned, code, sums, in_sem, w_sem, out_sem,
           sent, zr, yr, cr, fr, lr, gr, br, er):
    toks, width = tok.shape
    ff = wg.shape[1]
    me = lax.axis_index("ep")
    g, j = me // GROUP, me % GROUP
    partner = g * GROUP + (j + 1 - 2 * (j % 2))
    across = g * GROUP + (j + 2) % GROUP
    span = width // PIECES
    half = width // PARTS

    upper = (2 * g) // n
    edge = g + upper * (n - 1 - 2 * g)
    inner = 1 - 2 * upper

    def source(i):
        past = jnp.minimum(1, i // (2 * edge + 1))
        far = (1 - past) * ((i + 1) // 2) + past * (i - edge)
        way = past + (1 - past) * (2 * (i % 2) - 1)
        return g + inner * way * far

    def remote(src, dst, send, recv, device):
        return pltpu.make_async_remote_copy(
            src_ref=src, dst_ref=dst, send_sem=send, recv_sem=recv,
            device_id={"ep": device}, device_id_type=pl.DeviceIdType.MESH)

    barrier = pltpu.get_barrier_semaphore()
    others = [partner, across] + [source(i) * GROUP + j for i in range(1, n)]
    for other in others:
        pl.semaphore_signal(barrier, inc=1, device_id={"ep": other},
                            device_id_type=pl.DeviceIdType.MESH)

    inputs = [pltpu.make_async_copy(a, b, in_sem.at[k])
              for k, (a, b) in enumerate([(tok_in, tok), (gain_in, gain), (rt_in, rt), (gt_in, gt)])]
    for copy in inputs:
        copy.start()
    tiles = ff // LANE
    loads = []
    for t in range(tiles):
        loads.append(pltpu.make_async_copy(wg.at[:, pl.ds(t * LANE, LANE)], wgu.at[t, :, pl.ds(0, LANE)], w_sem.at[0]))
        loads.append(pltpu.make_async_copy(wu.at[:, pl.ds(t * LANE, LANE)], wgu.at[t, :, pl.ds(LANE, LANE)], w_sem.at[0]))
    loads.append(pltpu.make_async_copy(wd, wdn, w_sem.at[1]))
    table[...] = jnp.zeros_like(table)
    for copy in inputs[2:]:
        copy.wait()
    table[0:2] = rt[...].astype(jnp.float32)
    table[2:4] = gt[...]
    turned[...] = table[...].T
    experts_at = lax.broadcasted_iota(jnp.int32, (toks, LANE), 1).astype(jnp.float32)
    named = ((experts_at == turned[:, 0:1]) | (experts_at == turned[:, 1:2])).astype(jnp.float32)
    lower = (lax.broadcasted_iota(jnp.int32, (toks, toks), 1)
             < lax.broadcasted_iota(jnp.int32, (toks, toks), 0)).astype(jnp.bfloat16)
    before = jnp.dot(lower, named.astype(jnp.bfloat16), preferred_element_type=jnp.float32)
    code[...] = jnp.where(named > 0.5, before, -1.0)
    table[...] = code[...].T

    for copy in inputs[:2]:
        copy.wait()
    for copy in loads:
        copy.start()
    values = tok[...].astype(jnp.float32)
    scale = lax.rsqrt(jnp.mean(values * values, axis=-1, keepdims=True) + 1e-06)
    normed[...] = (values * scale * gain[...].reshape(1, width).astype(jnp.float32)).astype(jnp.bfloat16)

    def pack(e, dst):
        row = jnp.sum(jnp.where(lax.broadcasted_iota(jnp.int32, (LANE, toks), 0) == e, table[...], 0.0), axis=0, keepdims=True)
        slot = lax.broadcasted_iota(jnp.int32, (cap, toks), 0).astype(jnp.float32)
        pick = (slot == row).astype(jnp.bfloat16)
        for t in range(width // 512):
            cols = pl.ds(t * 512, 512)
            dst[:, cols] = jnp.dot(pick, normed[:, cols], preferred_element_type=jnp.float32).astype(jnp.bfloat16)

    def lane_rows(lane, count=1):
        return pl.ds(pl.multiple_of(lane * cap, cap), count * cap)

    def part_of(p):
        return pl.ds(p * half, half)

    def piece_of(h):
        return pl.ds(h * span, span)

    whole = pl.ds(0, width)

    def lane_copy(i, cols, src, dst, send, recv, device):
        s = source(i)
        return remote(xbuf.at[s, lane_rows(src), cols], xbuf.at[s, lane_rows(dst), cols], send, recv, device)

    def across_copy(i, p):
        return lane_copy(i, part_of(p), 0, 2, sent.at[0], yr.at[i, p], across)

    def beside_copy(i, cols):
        return lane_copy(i, cols, 0, 1, sent.at[1], cr.at[i], partner)

    def forward_copy(i, cols):
        return lane_copy(i, cols, 2, 3, sent.at[2], fr.at[i], partner)

    def last_forward(p):
        return lane_copy(n - 1, part_of(p), 2, 3, sent.at[2], fr.at[n - 1 + p], partner)

    def source_copy(i, p, to, at):
        return remote(outgoing.at[i, :, part_of(p)], xbuf.at[at, lane_rows(0), part_of(p)],
                      sent.at[3], zr.at[at, p], to * GROUP + j)

    def low_give(i, cols):
        return remote(give.at[i, 0, :, cols], take.at[i, 0, :, cols], sent.at[4], lr.at[i], partner)

    def high_give(i, p):
        return remote(give.at[i, 1, :, part_of(p)], take.at[i, 1, :, part_of(p)], sent.at[4], gr.at[i, p], partner)

    def cross_copy(i, h):
        return remote(cross.at[i, :, piece_of(h)], crossed.at[i, :, piece_of(h)],
                      sent.at[5], br.at[i, h], across)

    def return_copy(i, h, to, at):
        return remote(finished.at[i, :, piece_of(h)], ret.at[at, :, piece_of(h)],
                      sent.at[7 if i == n - 1 else 6], er.at[at, h], to * GROUP + j)

    def depart(i):
        for p in range(PARTS):
            source_copy(i, p, source(i), g).start()

    def relay(i, p):
        source_copy(i, p, partner // GROUP, source(i)).wait_recv()
        across_copy(i, p).start()
        beside_copy(i, part_of(p)).start()

    def forward(i, p):
        across_copy(i, p).wait_recv()
        forward_copy(i, part_of(p)).start()

    def rise(i, side):
        rows = xbuf[source(i), lane_rows(2 * side, 2)]
        for t in range(tiles):
            both = jnp.dot(rows, wgu[t], preferred_element_type=jnp.float32)
            gate_act, up_act = both[:, :LANE], both[:, LANE:]
            act = gate_act / (1.0 + jnp.exp(-gate_act)) * up_act
            hidden[:, pl.ds(t * LANE, LANE)] = act.astype(jnp.bfloat16)

    def rise_last():
        rows = xbuf.at[source(n - 1), lane_rows(2, 2)]
        for p in range(PARTS):
            across_copy(n - 1, p).wait_recv()
            last_forward(p).start()
            last_forward(p).wait_recv()
            block = rows[:, part_of(p)]
            for t in range(tiles):
                both = jnp.dot(block, wgu[t, part_of(p)], preferred_element_type=jnp.float32)
                cols = pl.ds(t * 2 * LANE, 2 * LANE)
                if p:
                    both = sums[:, cols] + both
                if p < PARTS - 1:
                    sums[:, cols] = both
                else:
                    gate_act, up_act = both[:, :LANE], both[:, LANE:]
                    act = gate_act / (1.0 + jnp.exp(-gate_act)) * up_act
                    hidden[:, pl.ds(t * LANE, LANE)] = act.astype(jnp.bfloat16)

    def fall(i, side):
        for p in parts:
            for h in groups[p]:
                cols = piece_of(h)
                piece = jnp.dot(hidden[...], wdn[:, cols], preferred_element_type=jnp.float32)
                part[i, side, :, cols] = piece[0:cap]
                give[i, side, :, cols] = piece[cap:2 * cap].astype(jnp.bfloat16)

            @pl.when(side == 0)
            def _():
                low_give(i, part_of(p)).start()

            @pl.when(side == 1)
            def _():
                high_give(i, p).start()

    def reduce_pair(i, h, send):
        for p in parts:
            if h == groups[p][0]:
                high_give(i, p).wait_recv()
        cols = piece_of(h)
        cross[i, :, cols] = (part[i, 1, :, cols] + take[i, 1, :, cols].astype(jnp.float32)).astype(jnp.bfloat16)
        if send:
            cross_copy(i, h).start()

    def send_cross(i, some):
        for h in some:
            cross_copy(i, h).start()

    def finish(i, h):
        if h == 0:
            low_give(i, whole).wait_recv()
        cross_copy(i, h).wait_recv()
        cols = piece_of(h)
        done = (part[i, 0, :, cols] + take[i, 0, :, cols].astype(jnp.float32)
                + crossed[i, :, cols].astype(jnp.float32)).astype(jnp.bfloat16)
        if i == 0:
            ret[g, :, cols] = done
        else:
            finished[i, :, cols] = done
            return_copy(i, h, source(i), g).start()

    def returned(i, h):
        return_copy(i, h, partner // GROUP, source(i)).wait_recv()

    def mixer(i):
        e = source(i)
        experts_at = lax.broadcasted_iota(jnp.int32, (toks, LANE), 1)
        column = jnp.sum(jnp.where(experts_at == e, code[...], 0.0), axis=1, keepdims=True)
        slot = lax.broadcasted_iota(jnp.int32, (toks, cap), 1).astype(jnp.float32)
        pick = (slot == column).astype(jnp.bfloat16)
        name = e.astype(jnp.float32)
        gate = (jnp.where(turned[:, 0:1] == name, turned[:, 2:3], 0.0)
                + jnp.where(turned[:, 1:2] == name, turned[:, 3:4], 0.0))
        def mix(h, start, last):
            cols = piece_of(h)
            if i:
                returned(i, h)
            term = gate * jnp.dot(pick, ret[e, :, cols], preferred_element_type=jnp.float32)
            if not start:
                term = total[:, cols] + term
            if last:
                out[:, cols] = term.astype(jnp.bfloat16)
                pltpu.make_async_copy(out.at[:, cols], out_to.at[:, cols], out_sem.at[0]).start()
            else:
                total[:, cols] = term

        return mix

    def mix_all(i, start, last):
        mix = mixer(i)
        for h in pieces:
            mix(h, start, last)

    def own(start, last):
        mix = mixer(0)
        for h in pieces:
            finish(0, h)
            mix(h, start, last)

    pieces = range(PIECES)
    parts = range(PARTS)
    groups = [pieces[p * PIECES // PARTS:(p + 1) * PIECES // PARTS] for p in parts]
    at_edge, within = edge == 0, edge > 0
    pack(g, xbuf.at[g, lane_rows(0)])
    pl.semaphore_wait(barrier, len(others))
    for p in parts:
        across_copy(0, p).start()
        beside_copy(0, part_of(p)).start()
    pack(source(1), outgoing.at[1])
    depart(1)
    for i in range(2, n):
        pack(source(i), outgoing.at[i])

        @pl.when(within)
        def _():
            depart(i)
    pltpu.make_async_copy(wgu, wgu, w_sem.at[0]).wait()
    loads[-1].wait()

    def step(k, carry):
        def at(c):
            return pl.when(k == c)

        def when_is(c):
            return (k == c).astype(jnp.int32)

        i = k // 2 + when_is(1) + when_is(3) - 2 * when_is(5)
        side = k % 2 + when_is(2) + when_is(4) - when_is(1) - when_is(3)

        @at(1)
        def _():
            for p in parts:
                forward(0, p)
                relay(1, p)

            @pl.when(within)
            def _():
                for p in parts:
                    relay(2, p)

        @at(2)
        def _():
            for p in parts:
                forward(1, p)

                @pl.when(at_edge)
                def _():
                    relay(2, p)
                    if p == 0:
                        for o in range(2, n):
                            depart(o)

        @at(4)
        def _():
            for p in parts:
                forward(2, p)

        for o in range(3, n):
            @at(2 * o - 1)
            def _():
                if o > 3:
                    for p in parts:
                        forward(o - 1, p)

                if o > 3:
                    @pl.when(within)
                    def _():
                        for p in parts:
                            relay(o, p)

            @at(2 * o)
            def _():
                for h in pieces[:-1]:
                    finish(o - 2, h)

                @pl.when(at_edge)
                def _():
                    relay(o, 0)
                finish(o - 2, PIECES - 1)

                @pl.when(at_edge)
                def _():
                    for p in parts[1:]:
                        relay(o, p)

        @pl.when(side == 0)
        def _():
            beside_copy(i, whole).wait_recv()

        @pl.when(side == 1)
        def _():
            forward_copy(i, whole).wait_recv()
        rise(i, side)

        for o in range(n - 1):
            @at(6 if o == 0 else 3 if o == 1 else 5 if o == 2 else 2 * o + 2)
            def _():
                for h in pieces[len(groups[0]):] if 0 < o < 3 else pieces:
                    reduce_pair(o, h, o > 0)
        fall(i, side)
        for o in (1, 2):
            @at(2 * o)
            def _():
                if o == 2:
                    @pl.when(within)
                    def _():
                        for p in parts:
                            relay(3, p)
                for h in groups[0]:
                    reduce_pair(o, h, True)
        return carry

    lax.fori_loop(0, 2 * n - 1, step, 0)

    first, last = pieces[:-2], PIECES - 1
    odd = j % 2 == 1

    @pl.when(at_edge)
    def _():
        send_cross(0, first)

        @pl.when(odd)
        def _():
            send_cross(0, [last - 1])
        for h in pieces:
            finish(n - 2, h)
    rise_last()

    @pl.when(within)
    def _():
        finish(n - 2, 0)
    fall(n - 1, 1)
    def drain():
        lane = [xbuf.at[:, lane_rows(k)] for k in range(3)]
        left = pl.ds(1, n - 1)
        for k, (src, dst) in enumerate([
                (lane[0], lane[2]), (lane[0], lane[1]), (lane[2], lane[1]),
                (outgoing.at[left], outgoing.at[left]), (give, take), (cross, crossed),
                (finished.at[pl.ds(1, n - 2)], ret.at[pl.ds(1, n - 2)])]):
            remote(src, dst, sent.at[k], yr.at[0, 0], partner).wait_send()

    @pl.when(at_edge)
    def _():
        for h in pieces:
            reduce_pair(n - 1, h, True)
        @pl.when(jnp.logical_not(odd))
        def _():
            send_cross(0, [last - 1])
        send_cross(0, [last])
        mixers = [mixer(i) for i in range(n)]
        for h in first:
            finish(0, h)
            mixers[0](h, True, False)
        for h in pieces:
            finish(n - 1, h)
        for h in pieces:
            if h not in first:
                finish(0, h)
                mixers[0](h, True, False)
            if h == last:
                drain()
            for mix in mixers[1:]:
                mix(h, False, mix is mixers[-1])

    @pl.when(within)
    def _():
        finish(n - 2, 1)
        for h in pieces:
            reduce_pair(n - 1, h, True)
        send_cross(0, pieces)
        for h in pieces[2:]:
            finish(n - 2, h)
        for h in pieces:
            finish(n - 1, h)
        for i in range(1, n):
            mix_all(i, i == 1, False)
        own(False, True)
        drain()
    remote(finished.at[n - 1], ret.at[0], sent.at[7], er.at[0, 0], partner).wait_send()
    pltpu.make_async_copy(out, out_to, out_sem.at[0]).wait()


def per_device(tokens, routing, gates, norm_gain, w_gate, w_up, w_down):
    toks, width = tokens.shape
    top = routing.shape[1]
    devices = lax.axis_size("ep")
    n = devices // GROUP
    cap = GROUP * (5 * toks * top // (4 * devices))
    cap = -(-cap // 16) * 16
    ff = w_gate.shape[2]
    bf, f32 = jnp.bfloat16, jnp.float32
    dma = pltpu.SemaphoreType.DMA
    hbm = pl.BlockSpec(memory_space=pl.ANY)
    return pl.pallas_call(
        functools.partial(kernel, n, cap),
        out_shape=jax.ShapeDtypeStruct((toks, width), bf),
        in_specs=[hbm] * 7,
        out_specs=hbm,
        scratch_shapes=[
            pltpu.VMEM((toks, width), bf),
            pltpu.VMEM((top, toks), jnp.int32),
            pltpu.VMEM((top, toks), f32),
            pltpu.VMEM((width,), bf),
            pltpu.VMEM((toks, width), bf),
            pltpu.VMEM((toks, width), bf),
            pltpu.VMEM((n, cap, width), bf),
            pltpu.VMEM((n, GROUP * cap, width), bf),
            pltpu.VMEM((ff // LANE, width, 2 * LANE), bf),
            pltpu.VMEM((ff, width), bf),
            pltpu.VMEM((2 * cap, ff), bf),
            pltpu.VMEM((n, 2, cap, width), f32),
            pltpu.VMEM((n, 2, cap, width), bf),
            pltpu.VMEM((n, 2, cap, width), bf),
            pltpu.VMEM((n, cap, width), bf),
            pltpu.VMEM((n, cap, width), bf),
            pltpu.VMEM((n, cap, width), bf),
            pltpu.VMEM((n, cap, width), bf),
            pltpu.VMEM((toks, width), f32),
            pltpu.VMEM((LANE, toks), f32),
            pltpu.VMEM((toks, LANE), f32),
            pltpu.VMEM((toks, LANE), f32),
            pltpu.VMEM((2 * cap, 2 * ff), f32),
            dma((4,)), dma((2,)), dma((1,)), dma((8,)), dma((n, PARTS)), dma((n, PARTS)), dma((n,)), dma((n - 1 + PARTS,)),
            dma((n,)), dma((n, PARTS)), dma((n, PIECES)), dma((n, PIECES)),
        ],
        compiler_params=pltpu.CompilerParams(
            collective_id=0, has_side_effects=True, vmem_limit_bytes=62 * 1024 * 1024),
    )(tokens, routing.T, gates.T, norm_gain, w_gate.reshape(w_gate.shape[1:]),
      w_up.reshape(w_up.shape[1:]), w_down.reshape(w_down.shape[1:]))


def solution(mesh):
    placed = (
        P(("grp", "ep"), None),
        P(("grp", "ep"), None),
        P(("grp", "ep"), None),
        P(),
        P("ep", None, None),
        P("ep", None, None),
        P("ep", None, None),
    )
    return jax.shard_map(
        per_device, mesh=mesh, in_specs=placed, out_specs=P(("grp", "ep"), None), check_vma=False
    )
```
